32 devices in a mesh: sp: 8 (over z, x), tp: 4 (over y, core).
Axes of the slice: x: 2, y: 2, z: 4, core: 2. Of those that a mesh axis runs over, the one named last changes fastest.
Arguments:
- inputs: bfloat16 [3072, 2048], P('sp', 'tp'), may hold values from -6 to 6
- norm_gain: float32 [2048], replicated, may hold values from 0.1 to 1.9
- query_weight: bfloat16 [2048, 1024], P(None, 'tp')
- key_weight: bfloat16 [2048, 1024], P(None, 'tp'), may hold values from -0.15625 to 0.15625
- value_weight: bfloat16 [2048, 1024], P(None, 'tp'), may hold values from -0.125 to 0.125
- memory_query_weight: bfloat16 [2048, 1024], P(None, 'tp'), may hold values from -0.125 to 0.125
- memory_key_weight: bfloat16 [2048, 1024], P(None, 'tp'), may hold values from -0.125 to 0.125
- memory_value_weight: bfloat16 [2048, 1024], P(None, 'tp'), may hold values from -0.125 to 0.125
- input_gate_weight: bfloat16 [2048, 16], P(None, 'tp')
- forget_gate_weight: bfloat16 [2048, 16], P(None, 'tp'), may hold values from -0.3125 to 0.3125
- forget_bias: float32 [16], P('tp'), may hold values from 3 to 13
- decay_shift: float32 [3072, 16], P('sp', 'tp'), may hold values from -2 to 0, as said below
- lambdas: float32 [16], P('tp'), may hold values from 0.3 to 0.8
- head_gain: float32 [64], replicated, may hold values from 0.1 to 1.9
- out_weight_attention: bfloat16 [1024, 2048], P('tp'), may hold values from -0.125 to 0.125
- out_weight_memory: bfloat16 [1024, 2048], P('tp'), may hold values from -0.125 to 0.125
Outputs:
- combined: bfloat16 [3072, 2048], P('sp', 'tp')
The draws below stay inside these ranges and needn't reach their ends.
Inputs may be any that keep to these rules, and one draw needn't show every extreme that they name: `decay_shift`: never positive.
All inputs are finite; a program needn't handle non-finite values.
Results may differ from the reference program's by a relative error of at most 0.018.
The reference program's roundings to bfloat16 on the way count: a program that leaves them out, or rounds other values in their place, can miss the bound.
Values may be sent and summed in bfloat16 or wider, within the bound.
No kernel may reach another device: no remote copies, remote signals or barrier semaphores. Data moves between devices by JAX's collectives and lax.ppermute only.
A program may use at most 192 MiB of HBM per device.

```python
import math
import jax
import jax.numpy as jnp
from jax import lax

D = 2048
HEAD = 64
DD = 32
HD = 16
MATRIX_HEADS = 16
BLOCK = 64
SEQUENCE_TOKENS = 3072
N_TP = 4


def draw_query_weight(key, part):
    entries = jnp.clip(jax.random.normal(jax.random.fold_in(key, 11), (D, HD * HEAD), jnp.float32), -6.0, 6.0)
    entries = entries * (1.3 / D ** 0.5)
    return entries.astype(jnp.bfloat16)


def draw_input_gate_weight(key, part):
    entries = jnp.clip(jax.random.normal(jax.random.fold_in(key, 13), (D, MATRIX_HEADS), jnp.float32), -6.0, 6.0)
    entries = entries / D ** 0.5
    return entries.astype(jnp.bfloat16)


def draw_forget_bias(key, part):
    fast_share = 0.5
    fast_heads = jax.random.uniform(jax.random.fold_in(key, 21), (MATRIX_HEADS,), jnp.float32) < fast_share
    jitter = jax.random.uniform(jax.random.fold_in(key, 22), (MATRIX_HEADS,), jnp.float32)
    quick_bias = math.log(40.0) + jitter - 0.5
    slow_bias = math.log(float(SEQUENCE_TOKENS)) + 2.0 + jitter
    return jnp.where(fast_heads, quick_bias, slow_bias).astype(jnp.float32)


def draw_decay_shift(key, part):
    block_count = SEQUENCE_TOKENS // BLOCK
    factor = jnp.exp(jax.random.uniform(jax.random.fold_in(key, 31), (block_count, 1, MATRIX_HEADS), jnp.float32, math.log(0.3), math.log(5.0)))
    constant_level = -jnp.broadcast_to(factor, (block_count, BLOCK, MATRIX_HEADS)).reshape(SEQUENCE_TOKENS, MATRIX_HEADS) / SEQUENCE_TOKENS
    spike_row_list = jax.random.randint(jax.random.fold_in(key, 32), (4, MATRIX_HEADS), 0, SEQUENCE_TOKENS)
    spike_dropouts = jnp.log(jax.random.uniform(jax.random.fold_in(key, 33), (4, MATRIX_HEADS), jnp.float32, 0.4, 0.75))
    row_indices = jnp.arange(SEQUENCE_TOKENS, dtype=jnp.int32)[:, None, None]
    spike_events = jnp.sum(jnp.where(row_indices == spike_row_list[None], spike_dropouts[None], 0.0), axis=1)
    return jnp.maximum(constant_level + spike_events, -2.0).astype(jnp.float32)


def levels(own_key, extent, cuts, low, top_value):
    def one(position, parts):
        draws = jax.random.uniform(jax.random.fold_in(jax.random.fold_in(own_key, 6), position), (parts,), jnp.float32, low / len(cuts), top_value / len(cuts))
        return jnp.repeat(jnp.exp(draws), extent[position] // parts).reshape((-1,) + (1,) * (len(extent) - position - 1))

    gain = one(*cuts[0])
    for cut in cuts[1:]:
        gain = gain * one(*cut)
    return gain


def centred(own_key, extent, deviation, bound, shards=(), kind=jnp.bfloat16):
    drawn = deviation * jax.random.normal(own_key, extent, jnp.float32)
    if shards:
        drawn = drawn * levels(own_key, extent, shards, -0.22, 0.18)
    return jnp.clip(drawn, -bound, bound).astype(kind)


def setup_inputs(seed: int = 0) -> dict:
    key_of = jax.random.split(jax.random.key(seed), 17)
    return {
        "inputs": centred(key_of[0], (SEQUENCE_TOKENS, D), 1.0, 6.0, ((0, 8), (1, 4))),
        "norm_gain": jnp.clip(1.0 + 0.18 * jax.random.normal(key_of[1], (D,), jnp.float32), 0.1, 1.9),
        "query_weight": draw_query_weight(jax.random.fold_in(key_of[16], 71), 0),
        "key_weight": centred(key_of[3], (D, HD * HEAD), (D * 10 // 17) ** -0.5, 0.15625, ((1, 4),)),
        "value_weight": centred(key_of[4], (D, HD * HEAD), D ** -0.5, 0.125, ((1, 4),)),
        "memory_query_weight": centred(key_of[5], (D, MATRIX_HEADS * HEAD), D ** -0.5, 0.125, ((1, 4),)),
        "memory_key_weight": centred(key_of[6], (D, MATRIX_HEADS * HEAD), D ** -0.5, 0.125, ((1, 4),)),
        "memory_value_weight": centred(key_of[7], (D, MATRIX_HEADS * HEAD), D ** -0.5, 0.125, ((1, 4),)),
        "input_gate_weight": draw_input_gate_weight(jax.random.fold_in(key_of[16], 71), 0),
        "forget_gate_weight": centred(key_of[9], (D, MATRIX_HEADS), (D // 6) ** -0.5, 0.3125, ((1, 4),)),
        "forget_bias": draw_forget_bias(jax.random.fold_in(key_of[16], 71), 0),
        "decay_shift": draw_decay_shift(jax.random.fold_in(key_of[16], 71), 0),
        "lambdas": jnp.clip(0.3 + 0.5 * jax.random.uniform(key_of[12], (HD,), jnp.float32) ** levels(key_of[12], (HD,), ((0, 4),), -0.2, 0.2), 0.3, 0.8),
        "head_gain": jnp.clip(1.0 + 0.18 * jax.random.normal(key_of[13], (HEAD,), jnp.float32), 0.1, 1.9),
        "out_weight_attention": centred(key_of[14], (HD * HEAD, D), ((HD + MATRIX_HEADS) * HEAD) ** -0.5, 0.125, ((0, 4),)),
        "out_weight_memory": centred(key_of[15], (MATRIX_HEADS * HEAD, D), ((HD + MATRIX_HEADS) * HEAD) ** -0.5, 0.125, ((0, 4),)),
    }


EPSILON = 1e-06
ROTARY_BASE = 10000.0
NEGATIVE = -1e+30

def rotate(halves, positions):
    middle = halves.shape[-1] // 2
    inverse = 1.0 / ROTARY_BASE ** (jnp.arange(middle, dtype=jnp.float32) / middle)
    angles = positions.astype(jnp.float32)[:, None] * inverse[None, :]
    cosine = jnp.cos(angles)[:, None, :]
    sine_part = jnp.sin(angles)[:, None, :]
    floats = halves.astype(jnp.float32)
    former = floats[..., :middle]
    latter = floats[..., middle:]
    turned = jnp.concatenate([former * cosine - latter * sine_part, latter * cosine + former * sine_part], axis=-1)
    return turned.astype(jnp.bfloat16)

def advance_state(carried, block_entry):
    memory, normal, stable = carried
    block_memory, block_normal, block_max, block_decay = block_entry
    new_stable = jnp.maximum(block_decay + stable, block_max)
    former = jnp.exp(block_decay + stable - new_stable)
    latter = jnp.exp(block_max - new_stable)
    return (former[:, None, None] * memory + latter[:, None, None] * block_memory, former[:, None] * normal + latter[:, None] * block_normal, new_stable)

def memory_blocks(queries, key_heads, values, gate_in, log_forget, entering):
    token_count, head_count, head_width = queries.shape
    block_count = token_count // BLOCK
    highest = lax.Precision.HIGHEST

    def blocked(flat_array):
        return flat_array.astype(jnp.float32).reshape(block_count, BLOCK, head_count, head_width).transpose(2, 0, 1, 3)
    query_blocks = blocked(queries)
    key_blocks = blocked(key_heads) * head_width ** (-0.5)
    value_blocks = blocked(values)
    gate_blocks = gate_in.reshape(block_count, BLOCK, head_count).transpose(2, 0, 1)
    cumulative = jnp.cumsum(log_forget.reshape(block_count, BLOCK, head_count).transpose(2, 0, 1), axis=-1)
    block_ends = cumulative[..., -1]
    toward_end = block_ends[..., None] - cumulative + gate_blocks
    local_max = lax.optimization_barrier(jnp.max(toward_end, axis=-1))
    end_weights = jnp.exp(toward_end - local_max[..., None])
    local_memory = jnp.einsum('hcl,hclv,hclk->chvk', end_weights, value_blocks, key_blocks, precision=highest)
    local_normal = jnp.einsum('hcl,hclk->chk', end_weights, key_blocks, precision=highest)

    def scan_step(carried, block_entry):
        return (advance_state(carried, block_entry), carried)
    entries = (local_memory, local_normal, local_max.T, block_ends.T)
    unused, (memory_in, normal_in, stable_in) = lax.scan(scan_step, entering, entries)
    lower_mask = jnp.tril(jnp.ones((BLOCK, BLOCK), dtype=bool))
    decays = jnp.where(lower_mask, cumulative[..., :, None] - cumulative[..., None, :] + gate_blocks[..., None, :], NEGATIVE)
    carried_log = cumulative + stable_in.T[..., None]
    row_max = jnp.maximum(carried_log, lax.optimization_barrier(jnp.max(decays, axis=-1)))
    within = jnp.where(lower_mask, jnp.exp(decays - row_max[..., None]), 0.0)
    outside = jnp.exp(carried_log - row_max)
    scores = within * jnp.einsum('hctd,hcsd->hcts', query_blocks, key_blocks, precision=highest)
    numerator = outside[..., None] * jnp.einsum('chvk,hctk->hctv', memory_in, query_blocks, precision=highest)
    numerator = numerator + jnp.einsum('hcts,hcsv->hctv', scores, value_blocks, precision=highest)
    denominator = outside * jnp.einsum('chk,hctk->hct', normal_in, query_blocks, precision=highest) + lax.optimization_barrier(jnp.sum(scores, axis=-1))
    result = numerator / jnp.maximum(jnp.abs(denominator), 1.0)[..., None]
    return result.transpose(1, 2, 0, 3).reshape(token_count, head_count * head_width).astype(jnp.bfloat16)

def differential(query_first, query_second, key_first, key_second, values, lambdas, head_gain):
    token_count = query_first.shape[0]
    query_span = min(512, token_count)
    score_scale = DD ** (-0.5)
    key_positions = jnp.arange(token_count, dtype=jnp.int32)

    def per_head(head_entry):
        head_query_first, head_query_second, head_key_first, head_key_second, value_head, factor = head_entry

        def per_block(block_index):
            first_row = block_index * query_span
            query_positions = first_row + jnp.arange(query_span, dtype=jnp.int32)
            visible = key_positions[None, :] <= query_positions[:, None]
            results = []
            for query_side, key_side in ((head_query_first, head_key_first), (head_query_second, head_key_second)):
                query_block = lax.dynamic_slice_in_dim(query_side, first_row, query_span, 0)
                scores = jnp.dot(query_block, key_side.T, preferred_element_type=jnp.float32) * score_scale
                scores = jnp.where(visible, scores, NEGATIVE)
                row_max = lax.optimization_barrier(jnp.max(scores, axis=1, keepdims=True))
                weights = jnp.where(visible, jnp.exp(scores - row_max), 0.0)
                totals = lax.optimization_barrier(jnp.sum(weights, axis=1, keepdims=True))
                results.append(jnp.dot(weights.astype(jnp.bfloat16), value_head, preferred_element_type=jnp.float32) / totals)
            return results[0] - factor * results[1]
        return lax.map(per_block, jnp.arange(token_count // query_span, dtype=jnp.int32))
    entries = (query_first.transpose(1, 0, 2), query_second.transpose(1, 0, 2), key_first.transpose(1, 0, 2), key_second.transpose(1, 0, 2), values.transpose(1, 0, 2), lambdas)
    stacked = lax.map(per_head, entries)
    head_count = stacked.shape[0]
    stacked = stacked.reshape(head_count, token_count, -1).transpose(1, 0, 2)
    norm_scale = lax.rsqrt(lax.optimization_barrier(jnp.mean(stacked * stacked, axis=-1, keepdims=True)) + EPSILON)
    return (stacked * norm_scale * head_gain).astype(jnp.bfloat16).reshape(token_count, -1)

def reference(inputs, norm_gain, query_weight, key_weight, value_weight, memory_query_weight, memory_key_weight, memory_value_weight, input_gate_weight, forget_gate_weight, forget_bias, decay_shift, lambdas, head_gain, out_weight_attention, out_weight_memory):
    token_count = inputs.shape[0]
    floats = inputs.astype(jnp.float32)
    inverse_rms = lax.rsqrt(lax.optimization_barrier(jnp.mean(floats * floats, axis=1, keepdims=True)) + EPSILON)
    scaled = (floats * norm_gain[None, :]).astype(jnp.bfloat16)

    def project(weight):
        return jnp.dot(scaled, weight, preferred_element_type=jnp.float32) * inverse_rms

    def split_heads(weight):
        return project(weight).astype(jnp.bfloat16).reshape(token_count, -1, HEAD)
    positions = jnp.arange(token_count, dtype=jnp.int32)
    queries = split_heads(query_weight)
    key_heads = split_heads(key_weight)
    values = split_heads(value_weight)
    attended = differential(rotate(queries[..., :DD], positions), rotate(queries[..., DD:], positions), rotate(key_heads[..., :DD], positions), rotate(key_heads[..., DD:], positions), values, lambdas, head_gain)
    gate_in = project(input_gate_weight)
    log_forget = jax.nn.log_sigmoid(project(forget_gate_weight) + forget_bias[None, :]) + decay_shift
    head_count = gate_in.shape[1]
    entering = (jnp.zeros((head_count, HEAD, HEAD), jnp.float32), jnp.zeros((head_count, HEAD), jnp.float32), jnp.zeros((head_count,), jnp.float32))
    memory = memory_blocks(split_heads(memory_query_weight), split_heads(memory_key_weight), split_heads(memory_value_weight), gate_in, log_forget, entering)
    attended_width = attended.shape[1] // N_TP
    memory_width = memory.shape[1] // N_TP
    combined = jnp.zeros((token_count, out_weight_attention.shape[1]), jnp.float32)
    for group_index in range(N_TP):
        low_a = group_index * attended_width
        low_m = group_index * memory_width
        partial_sum = jnp.dot(attended[:, low_a:low_a + attended_width], out_weight_attention[low_a:low_a + attended_width], preferred_element_type=jnp.float32)
        partial_sum = partial_sum + jnp.dot(memory[:, low_m:low_m + memory_width], out_weight_memory[low_m:low_m + memory_width], preferred_element_type=jnp.float32)
        combined = combined + lax.optimization_barrier(partial_sum.astype(jnp.bfloat16)).astype(jnp.float32)
    return combined.astype(jnp.bfloat16)
```

```python
import functools
import math

import jax
import jax.numpy as jnp
from jax import lax
from jax.experimental import pallas as pl
from jax.experimental.pallas import tpu as pltpu
from jax.sharding import PartitionSpec as P

EPSILON = 1e-06
ROTARY_BASE = 10000.0
NEGATIVE = -1e30
F32 = jnp.float32
BF16 = jnp.bfloat16
STATE_PAD = 16


def dot(a, b, contract, precision=None):
    return lax.dot_general(
        a, b, ((contract[:1], contract[1:]), ((), ())),
        preferred_element_type=F32, precision=precision,
    )


def call(body, out, args, flops, smem=(), scratch=()):
    vmem = pl.BlockSpec(memory_space=pltpu.VMEM)
    specs = [
        pl.BlockSpec(memory_space=pltpu.SMEM) if i in smem else vmem for i in range(len(args))
    ]
    return pl.pallas_call(
        body,
        out_shape=out,
        in_specs=specs,
        out_specs=jax.tree.map(lambda _: vmem, out),
        scratch_shapes=scratch,
        cost_estimate=pl.CostEstimate(flops=int(flops), bytes_accessed=1 << 20, transcendentals=0),
        compiler_params=pltpu.CompilerParams(vmem_limit_bytes=60 << 20),
    )(*args)


def shape(dims, kind):
    return jax.ShapeDtypeStruct(dims, kind)


def rotated(turned, cosine, sine, base, half):
    former = turned[base : base + half]
    latter = turned[base + half : base + 2 * half]
    return (
        (former * cosine - latter * sine).astype(BF16),
        (latter * cosine + former * sine).astype(BF16),
    )


def project(scaled, inverse, weight_ref, tp):
    total = None
    for k, piece in enumerate(scaled):
        term = dot(piece, weight_ref[tp ^ k], (1, 0))
        total = term if total is None else total + term
    return (total * inverse).astype(BF16).astype(F32).T


def kv_body(parts, head, *refs):
    pieces = refs[:parts]
    gain_ref, key_ref, value_ref, turn_ref = refs[parts : parts + 4]
    mine_ref, sent_ref, scaled_ref, inverse_ref = refs[parts + 4 :]
    tp = lax.axis_index("tp")
    odd = lax.rem(lax.axis_index("sp"), 2)
    squares = None
    scaled = []
    for k, piece in enumerate(pieces):
        floats = piece[...].astype(F32)
        term = jnp.sum(floats * floats, axis=1, keepdims=True)
        squares = term if squares is None else squares + term
        scaled.append((floats * gain_ref[tp ^ k]).astype(BF16))
        scaled_ref[k] = scaled[-1]
    features = parts * pieces[0].shape[1]
    inverse = lax.rsqrt(squares / features + EPSILON)
    inverse_ref[...] = jnp.broadcast_to(inverse, inverse_ref.shape)
    keys = project(scaled, inverse, key_ref, tp)
    values = project(scaled, inverse, value_ref, tp)
    half = head // 4
    cosine, sine = turn_ref[:half], turn_ref[half:]
    count = mine_ref.shape[0]
    for h in range(count):
        lots = []
        for group in range(2):
            base = (group * count + h) * head
            rows = []
            for side in range(2):
                rows.extend(rotated(keys, cosine, sine, base + side * 2 * half, half))
            rows.append(values[base : base + head].astype(BF16))
            lots.append(rows)
        at = 0
        for low, high in zip(*lots):
            size = low.shape[0]
            mine_ref[h, at : at + size] = jnp.where(odd == 0, low, high)
            sent_ref[h, at : at + size] = jnp.where(odd == 0, high, low)
            at += size


def rest_body(head, *refs):
    (scaled_ref, inverse_ref, query_ref, mq_ref, mk_ref, mv_ref, gate_ref, bias_ref, shift_ref,
     turn_ref, mine_ref, sent_ref, mqo_ref, mko_ref, mvo_ref, rows_ref, state_ref) = refs
    parts = scaled_ref.shape[0]
    tp = lax.axis_index("tp")
    odd = lax.rem(lax.axis_index("sp"), 2)
    scaled = [scaled_ref[k] for k in range(parts)]
    inverse = inverse_ref[:, :1]
    half = head // 4
    cosine, sine = turn_ref[:half], turn_ref[half:]
    queries = project(scaled, inverse, query_ref, tp)
    count = mine_ref.shape[0]
    for h in range(count):
        lots = []
        for group in range(2):
            base = (group * count + h) * head
            rows = []
            for side in range(2):
                rows.extend(rotated(queries, cosine, sine, base + side * 2 * half, half))
            lots.append(rows)
        for j, (low, high) in enumerate(zip(*lots)):
            mine_ref[h, j * half : (j + 1) * half] = jnp.where(odd == 0, low, high)
            sent_ref[h, j * half : (j + 1) * half] = jnp.where(odd == 0, high, low)
    mqo_ref[...] = project(scaled, inverse, mq_ref, tp).astype(BF16)
    memory_keys = project(scaled, inverse, mk_ref, tp)
    mko_ref[...] = memory_keys.astype(BF16)
    memory_values = project(scaled, inverse, mv_ref, tp)
    mvo_ref[...] = memory_values.astype(BF16)
    gates = None
    for k in range(parts):
        term = dot(scaled[k], gate_ref[tp ^ k], (1, 1))
        gates = term if gates is None else gates + term
    gates = (gates * inverse).T
    slots = shift_ref.shape[0]
    gate_in = gates[:slots]
    pre = gates[slots : 2 * slots] + bias_ref[...]
    log_forget = jnp.minimum(pre, 0.0) - jnp.log1p(jnp.exp(-jnp.abs(pre))) + shift_ref[...]
    row_count = log_forget.shape[1]
    upper = lax.broadcasted_iota(jnp.int32, (row_count, row_count), 0) <= lax.broadcasted_iota(
        jnp.int32, (row_count, row_count), 1
    )
    cumulative = dot(log_forget, upper.astype(F32), (1, 0), lax.Precision.HIGHEST)
    rows_ref[0] = gate_in
    rows_ref[1] = cumulative
    ending = jnp.sum(log_forget, axis=1, keepdims=True)
    toward = ending - cumulative + gate_in
    top = jnp.max(toward, axis=1, keepdims=True)
    weights = jnp.exp(toward - top)
    heads = memory_values.shape[0] // head
    for h in range(heads):
        keys = memory_keys[h * head : (h + 1) * head] * head**-0.5
        weight = weights[h : h + 1]
        left = jnp.concatenate(
            [
                memory_values[h * head : (h + 1) * head] * weight,
                jnp.broadcast_to(weight, (8, row_count)),
            ],
            axis=0,
        )
        local = dot(left, keys, (1, 1), lax.Precision.HIGHEST)
        marks = jnp.where(
            lax.broadcasted_iota(jnp.int32, (8, head), 0) < 4, top[h : h + 1], ending[h : h + 1]
        )
        lane = (h % 2) * head
        state_ref[h // 2, : head + 8, lane : lane + head] = local
        state_ref[h // 2, head + 8 :, lane : lane + head] = marks


def combine(earlier, later, head):
    stable, decay = earlier[head + 8 : head + 9], earlier[head + 12 : head + 13]
    next_stable, next_decay = later[head + 8 : head + 9], later[head + 12 : head + 13]
    top = jnp.maximum(next_decay + stable, next_stable)
    former = jnp.exp(next_decay + stable - top)
    latter = jnp.exp(next_stable - top)
    body = former * earlier[: head + 8] + latter * later[: head + 8]
    marks = jnp.where(
        lax.broadcasted_iota(jnp.int32, (8, body.shape[1]), 0) < 4, top, decay + next_decay
    )
    return jnp.concatenate([body, marks], axis=0)


def advance_body(head, entering_ref, own_ref, partner_ref, out_ref):
    odd = lax.rem(lax.axis_index("sp"), 2)
    for p in range(own_ref.shape[0]):
        own, partner = own_ref[p], partner_ref[p]
        first = jnp.where(odd == 0, own, partner)
        second = jnp.where(odd == 0, partner, own)
        out_ref[p] = combine(combine(entering_ref[p], first, head), second, head)


def split(value):
    high = value.astype(BF16)
    return high, (value - high.astype(F32)).astype(BF16)


def memory_body(head, mq_ref, mk_ref, mv_ref, rows_ref, entering_ref, partner_ref, out_ref):
    odd = lax.rem(lax.axis_index("sp"), 2)
    row_count = mq_ref.shape[1]
    gate_in, cumulative = rows_ref[0], rows_ref[1]
    slots = gate_in.shape[0]
    source = gate_in - cumulative
    filled = jnp.concatenate([source] * (128 // slots), axis=0).T
    visible = lax.broadcasted_iota(jnp.int32, (row_count, row_count), 0) <= lax.broadcasted_iota(
        jnp.int32, (row_count, row_count), 1
    )
    heads = mq_ref.shape[0] // head
    for h in range(heads):
        if h % 2 == 0:
            entering = entering_ref[h // 2]
            state = jnp.where(odd == 0, entering, combine(entering, partner_ref[h // 2], head))
        lane = (h % 2) * head
        body = state[: head + 8, lane : lane + head]
        stable = state[head + 8 : head + 9, lane : lane + 1]
        queries = mq_ref[h * head : (h + 1) * head]
        keys = mk_ref[h * head : (h + 1) * head]
        values = mv_ref[h * head : (h + 1) * head]
        row = cumulative[h : h + 1]
        gaps = jnp.where(visible, row + filled[:, h : h + 1], NEGATIVE)
        carried = row + stable
        top = jnp.maximum(carried, jnp.max(gaps, axis=0, keepdims=True))
        scores = jnp.exp(gaps - top) * (dot(keys, queries, (0, 0)) * head**-0.5)
        outside = jnp.exp(carried - top)
        high, low = split(body)
        past = (dot(high, queries, (1, 0)) + dot(low, queries, (1, 0))) * outside
        high, low = split(scores)
        numerator = past[:head] + dot(values, high, (1, 0)) + dot(values, low, (1, 0))
        denominator = past[head : head + 1] + jnp.sum(scores, axis=0, keepdims=True)
        result = numerator / jnp.maximum(jnp.abs(denominator), 1.0)
        out_ref[h * head : (h + 1) * head] = result.astype(BF16)


def attend(query, block, carried, head, mask):
    scale = (head // 2) ** -0.5 * math.log2(math.e)
    half = head // 2
    results = []
    values = block[head:]
    for side in range(2):
        top, total, sums = carried[side]
        scores = dot(block[side * half : (side + 1) * half], query[side * half : (side + 1) * half], (0, 0))
        if mask is not None:
            scores = jnp.where(mask, scores, NEGATIVE)
        new_top = jnp.max(scores, axis=0, keepdims=True)
        if top is not None:
            new_top = jnp.maximum(top, new_top)
        weights = jnp.exp2((scores - new_top) * scale)
        new_total = jnp.sum(weights, axis=0, keepdims=True)
        new_sums = dot(values, weights.astype(BF16), (1, 0))
        if top is not None:
            alpha = jnp.exp2((top - new_top) * scale)
            new_total = total * alpha + new_total
            new_sums = sums * alpha + new_sums
        results.append((new_top, new_total, new_sums))
    return results


def load(marks_ref, sums_ref, q, h, count):
    slot = q * count + h
    return [
        (marks_ref[slot, 2 * s : 2 * s + 1], marks_ref[slot, 2 * s + 1 : 2 * s + 2], sums_ref[slot, s])
        for s in range(2)
    ]


def store(marks_ref, sums_ref, q, h, count, results):
    slot = q * count + h
    for s, (top, total, sums) in enumerate(results):
        marks_ref[slot, 2 * s : 2 * s + 1] = top
        marks_ref[slot, 2 * s + 1 : 2 * s + 2] = total
        sums_ref[slot, s] = sums


def near_body(head, own_q, partner_q, own_kv, partner_kv, marks_ref, sums_ref):
    odd = lax.rem(lax.axis_index("sp"), 2)
    count, _, row_count = own_q.shape
    mask = lax.broadcasted_iota(jnp.int32, (row_count, row_count), 0) <= lax.broadcasted_iota(
        jnp.int32, (row_count, row_count), 1
    )
    marks_ref[...] = jnp.zeros_like(marks_ref)
    for q, (query, same, other) in enumerate(
        ((own_q, own_kv, partner_kv), (partner_q, partner_kv, own_kv))
    ):
        for h in range(count):
            results = attend(query[h], same[h], [(None, None, None)] * 2, head, mask)
            store(marks_ref, sums_ref, q, h, count, results)

        @pl.when(odd == 1 - q)
        def _():
            for h in range(count):
                results = attend(query[h], other[h], load(marks_ref, sums_ref, q, h, count), head, None)
                store(marks_ref, sums_ref, q, h, count, results)


def far_body(head, hop, own_q, partner_q, own_kv, partner_kv, marks_in, sums_in, marks_ref, sums_ref):
    count = own_q.shape[0]
    marks_ref[...] = marks_in[...]
    sums_ref[...] = sums_in[...]

    @pl.when(lax.axis_index("sp") // 2 >= hop)
    def _():
        for q, query in enumerate((own_q, partner_q)):
            for h in range(count):
                results = load(marks_ref, sums_ref, q, h, count)
                for block in (own_kv, partner_kv):
                    results = attend(query[h], block[h], results, head, None)
                store(marks_ref, sums_ref, q, h, count, results)


def last_body(head, marks_ref, sums_ref, lambda_ref, gain_ref, own_ref, partner_ref):
    odd = lax.rem(lax.axis_index("sp"), 2)
    count = own_ref.shape[0]
    for q, out in enumerate((own_ref, partner_ref)):
        for h in range(count):
            first, second = load(marks_ref, sums_ref, q, h, count)
            factor = lambda_ref[odd * count + h]
            difference = first[2] / first[1] - factor * (second[2] / second[1])
            square = jnp.mean(difference * difference, axis=0, keepdims=True)
            scaled = difference * lax.rsqrt(square + EPSILON) * gain_ref[...]
            out[h] = scaled.astype(BF16)


def out_body(head, chosen, own_ref, received_ref, memory_ref, wa_ref, wm_ref, *outs):
    tp = lax.axis_index("tp")
    odd = lax.rem(lax.axis_index("sp"), 2)
    count, _, row_count = own_ref.shape
    own = own_ref[...].reshape(count * head, row_count)
    received = received_ref[...].reshape(count * head, row_count)
    attended = jnp.concatenate(
        [jnp.where(odd == 0, own, received), jnp.where(odd == 0, received, own)], axis=0
    )
    memory = memory_ref[...]
    width = outs[0].shape[1]
    for k, out in zip(chosen, outs):
        columns = pl.ds(pl.multiple_of((tp ^ k) * width, 128), width)
        partial = dot(attended, wa_ref[:, columns], (0, 0)) + dot(memory, wm_ref[:, columns], (0, 0))
        out[...] = partial.astype(BF16)


def per_device(
    inputs, norm_gain, query_weight, key_weight, value_weight, memory_query_weight,
    memory_key_weight, memory_value_weight, input_gate_weight, forget_gate_weight, forget_bias,
    decay_shift, lambdas, head_gain, out_weight_attention, out_weight_memory, *, sp_size, tp_size,
):
    row_count, width = inputs.shape
    head = head_gain.shape[0]
    heads = query_weight.shape[1] // head
    memory_heads = memory_query_weight.shape[1] // head
    count = heads // 2
    sp = lax.axis_index("sp")

    def swap(array, axis, size, bit):
        return lax.ppermute(array, axis, [(j, j ^ bit) for j in range(size)])

    def onward(array, first):
        return lax.ppermute(array, "sp", [(j, j + 2) for j in range(2 * first, sp_size - 2)])

    pieces = [None] * tp_size
    pieces[0] = inputs
    for k in range(2, tp_size, 2):
        pieces[k] = swap(inputs, "tp", tp_size, k)
    for k in range(0, tp_size, 2):
        pieces[k + 1] = swap(pieces[k], "tp", tp_size, 1)

    quarter = head // 4
    rates = 1.0 / ROTARY_BASE ** (jnp.arange(quarter, dtype=F32) / quarter)
    positions = (sp * row_count + jnp.arange(row_count, dtype=jnp.int32)).astype(F32)
    angles = positions[None, :] * rates[:, None]
    turn = jnp.concatenate([jnp.cos(angles), jnp.sin(angles)], axis=0)

    def blocks(weight):
        return weight.reshape(tp_size, width, weight.shape[1])

    slots = 8
    gates = jnp.concatenate(
        [
            jnp.pad(input_gate_weight.T, ((0, slots - memory_heads), (0, 0))),
            jnp.pad(forget_gate_weight.T, ((0, 128 - slots - memory_heads), (0, 0))),
        ],
        axis=0,
    )
    gates = gates.reshape(128, tp_size, width).transpose(1, 0, 2)
    bias = jnp.pad(forget_bias, (0, slots - memory_heads))[:, None]
    shift = jnp.pad(decay_shift.T, ((0, slots - memory_heads), (0, 0)))

    kv_shape = shape((count, 2 * head, row_count), BF16)
    kv_own, kv_sent, scaled, inverse = call(
        functools.partial(kv_body, tp_size, head),
        (kv_shape, kv_shape, shape((tp_size, row_count, width), BF16), shape((row_count, 128), F32)),
        (*pieces, norm_gain.reshape(tp_size, 1, width), blocks(key_weight), blocks(value_weight), turn),
        2e9,
    )
    kv_partner = swap(kv_sent, "sp", sp_size, 1)
    chains = [(kv_own, kv_partner)]
    for hop in range(1, sp_size // 2):
        chains.append(tuple(onward(block, hop - 1) for block in chains[-1]))

    q_shape = shape((count, head, row_count), BF16)
    m_shape = shape((memory_heads * head, row_count), BF16)
    state_shape = shape((memory_heads // 2, head + STATE_PAD, 2 * head), F32)
    q_own, q_sent, mq, mk, mv, rows, state = call(
        functools.partial(rest_body, head),
        (q_shape, q_shape, m_shape, m_shape, m_shape, shape((2, slots, row_count), F32), state_shape),
        (scaled, inverse, blocks(query_weight), blocks(memory_query_weight), blocks(memory_key_weight),
         blocks(memory_value_weight), gates, bias, shift, turn),
        4e9,
    )
    q_partner = swap(q_sent, "sp", sp_size, 1)
    state_partner = swap(state, "sp", sp_size, 1)
    entering = jnp.zeros(state_shape.shape, F32)
    for hop in range(1, sp_size // 2):
        leaving = call(
            functools.partial(advance_body, head), state_shape, (entering, state, state_partner), 1e6
        )
        arrived = lax.ppermute(
            leaving, "sp", [(2 * hop - 2 + j, 2 * hop + j) for j in range(2)]
        )
        entering = jnp.where(sp // 2 == hop, arrived, entering)

    marks_shape = shape((2 * count, 8, row_count), F32)
    sums_shape = shape((2 * count, 2, head, row_count), F32)
    marks, sums = call(
        functools.partial(near_body, head), (marks_shape, sums_shape), (q_own, q_partner, *chains[0]), 2e9
    )
    memory = call(
        functools.partial(memory_body, head), m_shape, (mq, mk, mv, rows, entering, state_partner), 2e9
    )
    for hop in range(1, sp_size // 2):
        marks, sums = call(
            functools.partial(far_body, head, hop),
            (marks_shape, sums_shape),
            (q_own, q_partner, *chains[hop], marks, sums),
            3e9,
        )
    attended_own, attended_sent = call(
        functools.partial(last_body, head),
        (q_shape, q_shape),
        (marks, sums, lambdas, head_gain[:, None]),
        1e7,
        smem=(2,),
    )
    attended_received = swap(attended_sent, "sp", sp_size, 1)

    part_shape = shape((row_count, width), BF16)

    def partials(chosen):
        return call(
            functools.partial(out_body, head, chosen),
            tuple(part_shape for _ in chosen),
            (attended_own, attended_received, memory, out_weight_attention, out_weight_memory),
            5e8 * len(chosen),
        )

    chosen = tuple(range(2, tp_size))
    remote = dict(zip(chosen, partials(chosen)))
    arrivals = []
    for k in range(2, tp_size, 2):
        pair = swap(remote[k + 1], "tp", tp_size, 1)
        summed = (remote[k].astype(F32) + pair.astype(F32)).astype(BF16)
        arrivals.append(swap(summed, "tp", tp_size, k))
    kept, sent = partials((0, 1))
    total = kept.astype(F32) + swap(sent, "tp", tp_size, 1).astype(F32)
    for arrival in arrivals:
        total = total + arrival.astype(F32)
    return total.astype(BF16)


def solution(mesh):
    in_specs = (
        P("sp", "tp"), P(), P(None, "tp"), P(None, "tp"), P(None, "tp"), P(None, "tp"),
        P(None, "tp"), P(None, "tp"), P(None, "tp"), P(None, "tp"), P("tp"), P("sp", "tp"),
        P("tp"), P(), P("tp", None), P("tp", None),
    )
    body = functools.partial(per_device, sp_size=mesh.shape["sp"], tp_size=mesh.shape["tp"])
    return jax.shard_map(
        body, mesh=mesh, in_specs=in_specs, out_specs=P("sp", "tp"), check_vma=False
    )
```

```python
import functools
import math

import jax
import jax.numpy as jnp
from jax import lax
from jax.experimental import pallas as pl
from jax.experimental.pallas import tpu as pltpu
from jax.sharding import PartitionSpec as P

EPSILON = 1e-06
ROTARY_BASE = 10000.0
NEGATIVE = -1e30
F32 = jnp.float32
BF16 = jnp.bfloat16
STATE_PAD = 16


def dot(a, b, contract, precision=None):
    return lax.dot_general(
        a, b, ((contract[:1], contract[1:]), ((), ())),
        preferred_element_type=F32, precision=precision,
    )


def call(body, out, args, flops, mib=8, smem=(), scratch=()):
    vmem = pl.BlockSpec(memory_space=pltpu.VMEM)
    specs = [
        pl.BlockSpec(memory_space=pltpu.SMEM) if i in smem else vmem for i in range(len(args))
    ]
    return pl.pallas_call(
        body,
        out_shape=out,
        in_specs=specs,
        out_specs=jax.tree.map(lambda _: vmem, out),
        scratch_shapes=scratch,
        cost_estimate=pl.CostEstimate(flops=int(flops), bytes_accessed=1 << 20, transcendentals=0),
        compiler_params=pltpu.CompilerParams(vmem_limit_bytes=mib << 20),
    )(*args)


def shape(dims, kind):
    return jax.ShapeDtypeStruct(dims, kind)


def rotated(turned, cosine, sine, base, half):
    former = turned[base : base + half]
    latter = turned[base + half : base + 2 * half]
    return (
        (former * cosine - latter * sine).astype(BF16),
        (latter * cosine + former * sine).astype(BF16),
    )


def project(scaled, inverse, weight_ref, tp):
    total = None
    for k, piece in enumerate(scaled):
        term = dot(piece, weight_ref[tp ^ k], (1, 0))
        total = term if total is None else total + term
    return (total * inverse).astype(BF16).astype(F32).T


def kv_body(parts, head, *refs):
    pieces = refs[:parts]
    gain_ref, key_ref, value_ref, turn_ref = refs[parts : parts + 4]
    mine_ref, sent_ref, scaled_ref, inverse_ref = refs[parts + 4 :]
    tp = lax.axis_index("tp")
    odd = lax.rem(lax.axis_index("sp"), 2)
    squares = None
    scaled = []
    for k, piece in enumerate(pieces):
        floats = piece[...].astype(F32)
        term = jnp.sum(floats * floats, axis=1, keepdims=True)
        squares = term if squares is None else squares + term
        scaled.append((floats * gain_ref[tp ^ k]).astype(BF16))
        scaled_ref[k] = scaled[-1]
    features = parts * pieces[0].shape[1]
    inverse = lax.rsqrt(squares / features + EPSILON)
    inverse_ref[...] = jnp.broadcast_to(inverse, inverse_ref.shape)
    keys = project(scaled, inverse, key_ref, tp)
    values = project(scaled, inverse, value_ref, tp)
    half = head // 4
    cosine, sine = turn_ref[:half], turn_ref[half:]
    count = mine_ref.shape[0]
    for h in range(count):
        lots = []
        for group in range(2):
            base = (group * count + h) * head
            rows = []
            for side in range(2):
                rows.extend(rotated(keys, cosine, sine, base + side * 2 * half, half))
            rows.append(values[base : base + head].astype(BF16))
            lots.append(rows)
        at = 0
        for low, high in zip(*lots):
            size = low.shape[0]
            mine_ref[h, at : at + size] = jnp.where(odd == 0, low, high)
            sent_ref[h, at : at + size] = jnp.where(odd == 0, high, low)
            at += size


def rest_body(head, *refs):
    (scaled_ref, inverse_ref, query_ref, mq_ref, mk_ref, mv_ref, gate_ref, bias_ref, shift_ref,
     turn_ref, mine_ref, sent_ref, mqo_ref, mko_ref, mvo_ref, rows_ref, state_ref) = refs
    parts = scaled_ref.shape[0]
    tp = lax.axis_index("tp")
    odd = lax.rem(lax.axis_index("sp"), 2)
    scaled = [scaled_ref[k] for k in range(parts)]
    inverse = inverse_ref[:, :1]
    half = head // 4
    cosine, sine = turn_ref[:half], turn_ref[half:]
    queries = project(scaled, inverse, query_ref, tp)
    count = mine_ref.shape[0]
    for h in range(count):
        lots = []
        for group in range(2):
            base = (group * count + h) * head
            rows = []
            for side in range(2):
                rows.extend(rotated(queries, cosine, sine, base + side * 2 * half, half))
            lots.append(rows)
        for j, (low, high) in enumerate(zip(*lots)):
            mine_ref[h, j * half : (j + 1) * half] = jnp.where(odd == 0, low, high)
            sent_ref[h, j * half : (j + 1) * half] = jnp.where(odd == 0, high, low)
    mqo_ref[...] = project(scaled, inverse, mq_ref, tp).astype(BF16)
    memory_keys = project(scaled, inverse, mk_ref, tp)
    mko_ref[...] = memory_keys.astype(BF16)
    memory_values = project(scaled, inverse, mv_ref, tp)
    mvo_ref[...] = memory_values.astype(BF16)
    gates = None
    for k in range(parts):
        term = dot(scaled[k], gate_ref[tp ^ k], (1, 1))
        gates = term if gates is None else gates + term
    gates = (gates * inverse).T
    slots = shift_ref.shape[0]
    gate_in = gates[:slots]
    pre = gates[slots:] + bias_ref[...]
    log_forget = jnp.minimum(pre, 0.0) - jnp.log1p(jnp.exp(-jnp.abs(pre))) + shift_ref[...]
    row_count = log_forget.shape[1]
    upper = lax.broadcasted_iota(jnp.int32, (row_count, row_count), 0) <= lax.broadcasted_iota(
        jnp.int32, (row_count, row_count), 1
    )
    cumulative = dot(log_forget, upper.astype(F32), (1, 0), lax.Precision.HIGHEST)
    rows_ref[0] = gate_in
    rows_ref[1] = cumulative
    ending = jnp.sum(log_forget, axis=1, keepdims=True)
    toward = ending - cumulative + gate_in
    top = jnp.max(toward, axis=1, keepdims=True)
    weights = jnp.exp(toward - top)
    heads = memory_values.shape[0] // head
    for h in range(heads):
        keys = memory_keys[h * head : (h + 1) * head] * head**-0.5
        weight = weights[h : h + 1]
        left = jnp.concatenate(
            [
                memory_values[h * head : (h + 1) * head] * weight,
                jnp.broadcast_to(weight, (8, row_count)),
            ],
            axis=0,
        )
        local = dot(left, keys, (1, 1), lax.Precision.HIGHEST)
        marks = jnp.where(
            lax.broadcasted_iota(jnp.int32, (8, head), 0) < 4, top[h : h + 1], ending[h : h + 1]
        )
        lane = (h % 2) * head
        state_ref[h // 2, : head + 8, lane : lane + head] = local
        state_ref[h // 2, head + 8 :, lane : lane + head] = marks


def combine(earlier, later, head):
    stable, decay = earlier[head + 8 : head + 9], earlier[head + 12 : head + 13]
    next_stable, next_decay = later[head + 8 : head + 9], later[head + 12 : head + 13]
    top = jnp.maximum(next_decay + stable, next_stable)
    former = jnp.exp(next_decay + stable - top)
    latter = jnp.exp(next_stable - top)
    body = former * earlier[: head + 8] + latter * later[: head + 8]
    marks = jnp.where(
        lax.broadcasted_iota(jnp.int32, (8, body.shape[1]), 0) < 4, top, decay + next_decay
    )
    return jnp.concatenate([body, marks], axis=0)


def entered(refs, p):
    total = None
    for ref in refs:
        total = ref[p] if total is None else total + ref[p]
    return total


def advance_body(head, own_ref, partner_ref, *refs):
    entering_refs, out_ref = refs[:-1], refs[-1]
    odd = lax.rem(lax.axis_index("sp"), 2)
    for p in range(own_ref.shape[0]):
        own, partner = own_ref[p], partner_ref[p]
        first = jnp.where(odd == 0, own, partner)
        second = jnp.where(odd == 0, partner, own)
        entering = entered(entering_refs, p) if entering_refs else jnp.zeros_like(own)
        out_ref[p] = combine(combine(entering, first, head), second, head)


def split(value):
    high = value.astype(BF16)
    return high, (value - high.astype(F32)).astype(BF16)


def memory_body(head, mq_ref, mk_ref, mv_ref, rows_ref, partner_ref, *refs):
    entering_refs, out_ref = refs[:-1], refs[-1]
    odd = lax.rem(lax.axis_index("sp"), 2)
    row_count = mq_ref.shape[1]
    gate_in, cumulative = rows_ref[0], rows_ref[1]
    filled = (gate_in - cumulative).T
    visible = lax.broadcasted_iota(jnp.int32, (row_count, row_count), 0) <= lax.broadcasted_iota(
        jnp.int32, (row_count, row_count), 1
    )
    heads = mq_ref.shape[0] // head
    for h in range(heads):
        if h % 2 == 0:
            entering = entered(entering_refs, h // 2)
            state = jnp.where(odd == 0, entering, combine(entering, partner_ref[h // 2], head))
        lane = (h % 2) * head
        body = state[: head + 8, lane : lane + head]
        stable = state[head + 8 : head + 9, lane : lane + 1]
        queries = mq_ref[h * head : (h + 1) * head]
        keys = mk_ref[h * head : (h + 1) * head]
        values = mv_ref[h * head : (h + 1) * head]
        row = cumulative[h : h + 1]
        gaps = jnp.where(visible, row + filled[:, h : h + 1], NEGATIVE)
        carried = row + stable
        top = jnp.maximum(carried, jnp.max(gaps, axis=0, keepdims=True))
        scores = jnp.exp(gaps - top) * (dot(keys, queries, (0, 0)) * head**-0.5)
        outside = jnp.exp(carried - top)
        high, low = split(body)
        past = (dot(high, queries, (1, 0)) + dot(low, queries, (1, 0))) * outside
        high, low = split(scores)
        numerator = past[:head] + dot(values, high, (1, 0)) + dot(values, low, (1, 0))
        denominator = past[head : head + 1] + jnp.sum(scores, axis=0, keepdims=True)
        result = numerator / jnp.maximum(jnp.abs(denominator), 1.0)
        out_ref[h * head : (h + 1) * head] = result.astype(BF16)


def attend(query, blocks, carried, head, mask):
    scale = (head // 2) ** -0.5 * math.log2(math.e)
    scores = [dot(key, query, (0, 0)) for key, _ in blocks]
    if mask is not None:
        scores = [jnp.where(mask, score, NEGATIVE) for score in scores]
    tops = [jnp.max(score, axis=0, keepdims=True) for score in scores]
    if carried is not None:
        tops.append(carried[0])
    top = functools.reduce(jnp.maximum, tops)
    total, sums = None, None
    if carried is not None:
        alpha = jnp.exp2((carried[0] - top) * scale)
        total, sums = carried[1] * alpha, carried[2] * alpha
    for score, (_, value) in zip(scores, blocks):
        weights = jnp.exp2((score - top) * scale)
        more = jnp.sum(weights, axis=0, keepdims=True)
        sum_more = dot(value, weights.astype(BF16), (1, 0))
        total = more if total is None else total + more
        sums = sum_more if sums is None else sums + sum_more
    return top, total, sums


def halves(head, index):
    half = head // 2
    h, side = index // 2, lax.rem(index, 2)
    return h, pl.ds(pl.multiple_of(side * half, half), half)


def near_body(head, own_q, partner_q, own_kv, partner_kv, marks_ref, sums_ref):
    odd = lax.rem(lax.axis_index("sp"), 2)
    count, _, row_count = own_q.shape
    mask = lax.broadcasted_iota(jnp.int32, (row_count, row_count), 0) <= lax.broadcasted_iota(
        jnp.int32, (row_count, row_count), 1
    )
    for q, (query, same, other) in enumerate(
        ((own_q, own_kv, partner_kv), (partner_q, partner_kv, own_kv))
    ):
        lanes = slice(q * row_count, (q + 1) * row_count)

        def step(index, _):
            h, part = halves(head, index)
            top, total, sums = attend(
                query[h, part], [(same[h, part], same[h, head:])], None, head, mask
            )
            marks_ref[index, 0:1, lanes] = top
            marks_ref[index, 1:2, lanes] = total
            sums_ref[index, :, lanes] = sums
            return 0

        lax.fori_loop(0, 2 * count, step, 0)

        def more(index, _):
            h, part = halves(head, index)
            carried = (
                marks_ref[index, 0:1, lanes], marks_ref[index, 1:2, lanes], sums_ref[index, :, lanes]
            )
            top, total, sums = attend(
                query[h, part], [(other[h, part], other[h, head:])], carried, head, None
            )
            marks_ref[index, 0:1, lanes] = top
            marks_ref[index, 1:2, lanes] = total
            sums_ref[index, :, lanes] = sums
            return 0

        @pl.when(odd == 1 - q)
        def _():
            lax.fori_loop(0, 2 * count, more, 0)


def far_body(head, hop, final, own_q, partner_q, own_kv, partner_kv, marks_in, sums_in, *refs):
    count, _, row_count = own_q.shape
    if final:
        lambda_ref, gain_ref, own_ref, partner_ref, marks_ref, sums_ref = refs
    else:
        marks_ref, sums_ref = refs
    valid = lax.axis_index("sp") // 2 >= hop

    @pl.when(jnp.logical_not(valid))
    def _():
        marks_ref[...] = marks_in[...]
        sums_ref[...] = sums_in[...]

    @pl.when(valid)
    def _():
        def step(index, _):
            h, part = halves(head, index)
            query = jnp.concatenate([own_q[h, part], partner_q[h, part]], axis=1)
            carried = (marks_in[index, 0:1], marks_in[index, 1:2], sums_in[index])
            blocks = [(block[h, part], block[h, head:]) for block in (own_kv, partner_kv)]
            top, total, sums = attend(query, blocks, carried, head, None)
            marks_ref[index, 0:1] = top
            marks_ref[index, 1:2] = total
            sums_ref[index] = sums
            return 0

        lax.fori_loop(0, 2 * count, step, 0)

    if final:
        odd = lax.rem(lax.axis_index("sp"), 2)
        for h in range(count):
            first = sums_ref[2 * h] / marks_ref[2 * h, 1:2]
            second = sums_ref[2 * h + 1] / marks_ref[2 * h + 1, 1:2]
            difference = first - lambda_ref[odd * count + h] * second
            square = jnp.mean(difference * difference, axis=0, keepdims=True)
            scaled = (difference * lax.rsqrt(square + EPSILON) * gain_ref[...]).astype(BF16)
            own_ref[h] = scaled[:, :row_count]
            partner_ref[h] = scaled[:, row_count:]


def out_body(head, chosen, own_ref, received_ref, memory_ref, wa_ref, wm_ref, *outs):
    tp = lax.axis_index("tp")
    odd = lax.rem(lax.axis_index("sp"), 2)
    count, _, row_count = own_ref.shape
    own = own_ref[...].reshape(count * head, row_count)
    received = received_ref[...].reshape(count * head, row_count)
    attended = jnp.concatenate(
        [jnp.where(odd == 0, own, received), jnp.where(odd == 0, received, own)], axis=0
    )
    memory = memory_ref[...]
    width = outs[0].shape[1]
    for k, out in zip(chosen, outs):
        columns = pl.ds(pl.multiple_of((tp ^ k) * width, 128), width)
        partial = dot(attended, wa_ref[:, columns], (0, 0)) + dot(memory, wm_ref[:, columns], (0, 0))
        out[...] = partial.astype(BF16)


def per_device(
    inputs, norm_gain, query_weight, key_weight, value_weight, memory_query_weight,
    memory_key_weight, memory_value_weight, input_gate_weight, forget_gate_weight, forget_bias,
    decay_shift, lambdas, head_gain, out_weight_attention, out_weight_memory, *, sp_size, tp_size,
):
    row_count, width = inputs.shape
    head = head_gain.shape[0]
    heads = query_weight.shape[1] // head
    memory_heads = memory_query_weight.shape[1] // head
    count = heads // 2
    sp = lax.axis_index("sp")

    def swap(array, axis, size, bit):
        return lax.ppermute(array, axis, [(j, j ^ bit) for j in range(size)])

    def onward(array, first):
        return lax.ppermute(array, "sp", [(j, j + 2) for j in range(2 * first, sp_size - 2)])

    pieces = [None] * tp_size
    pieces[0] = inputs
    for k in range(2, tp_size, 2):
        pieces[k] = swap(inputs, "tp", tp_size, k)
    for k in range(0, tp_size, 2):
        pieces[k + 1] = swap(pieces[k], "tp", tp_size, 1)

    quarter = head // 4
    rates = 1.0 / ROTARY_BASE ** (jnp.arange(quarter, dtype=F32) / quarter)
    positions = (sp * row_count + jnp.arange(row_count, dtype=jnp.int32)).astype(F32)
    angles = positions[None, :] * rates[:, None]
    turn = jnp.concatenate([jnp.cos(angles), jnp.sin(angles)], axis=0)

    def blocks(weight):
        return weight.reshape(tp_size, width, weight.shape[1])

    gates = jnp.concatenate([input_gate_weight.T, forget_gate_weight.T], axis=0)
    gates = gates.reshape(2 * memory_heads, tp_size, width).transpose(1, 0, 2)
    bias = forget_bias[:, None]
    shift = decay_shift.T

    kv_shape = shape((count, 2 * head, row_count), BF16)
    kv_own, kv_sent, scaled, inverse = call(
        functools.partial(kv_body, tp_size, head),
        (kv_shape, kv_shape, shape((tp_size, row_count, width), BF16), shape((row_count, 128), F32)),
        (*pieces, norm_gain.reshape(tp_size, 1, width), blocks(key_weight), blocks(value_weight), turn),
        2e9,
    )
    kv_partner = swap(kv_sent, "sp", sp_size, 1)
    chains = [(kv_own, kv_partner)]
    for hop in range(1, sp_size // 2):
        chains.append(tuple(onward(block, hop - 1) for block in chains[-1]))

    q_shape = shape((count, head, row_count), BF16)
    m_shape = shape((memory_heads * head, row_count), BF16)
    state_shape = shape((memory_heads // 2, head + STATE_PAD, 2 * head), F32)
    q_own, q_sent, mq, mk, mv, rows, state = call(
        functools.partial(rest_body, head),
        (q_shape, q_shape, m_shape, m_shape, m_shape, shape((2, memory_heads, row_count), F32), state_shape),
        (scaled, inverse, blocks(query_weight), blocks(memory_query_weight), blocks(memory_key_weight),
         blocks(memory_value_weight), gates, bias, shift, turn),
        4e9,
    )
    q_partner = swap(q_sent, "sp", sp_size, 1)
    state_partner = swap(state, "sp", sp_size, 1)
    entering = []
    for hop in range(1, sp_size // 2):
        leaving = call(
            functools.partial(advance_body, head), state_shape, (state, state_partner, *entering), 1e6, 4
        )
        entering.append(
            lax.ppermute(leaving, "sp", [(2 * hop - 2 + j, 2 * hop + j) for j in range(2)])
        )

    marks_shape = shape((2 * count, 8, 2 * row_count), F32)
    sums_shape = shape((2 * count, head, 2 * row_count), F32)
    marks, sums = call(
        functools.partial(near_body, head), (marks_shape, sums_shape), (q_own, q_partner, *chains[0]), 2e9
    )
    memory = call(
        functools.partial(memory_body, head), m_shape, (mq, mk, mv, rows, state_partner, *entering), 2e9
    )
    last = sp_size // 2 - 1
    for hop in range(1, last):
        marks, sums = call(
            functools.partial(far_body, head, hop, False),
            (marks_shape, sums_shape),
            (q_own, q_partner, *chains[hop], marks, sums),
            3e9,
        )
    attended_own, attended_sent = call(
        functools.partial(far_body, head, last, True),
        (q_shape, q_shape),
        (q_own, q_partner, *chains[last], marks, sums, lambdas, head_gain[:, None]),
        3e9,
        smem=(6,),
        scratch=(pltpu.VMEM(marks_shape.shape, F32), pltpu.VMEM(sums_shape.shape, F32)),
    )
    attended_received = swap(attended_sent, "sp", sp_size, 1)

    part_shape = shape((row_count, width), BF16)

    def partials(chosen):
        return call(
            functools.partial(out_body, head, chosen),
            tuple(part_shape for _ in chosen),
            (attended_own, attended_received, memory, out_weight_attention, out_weight_memory),
            5e8 * len(chosen),
        )

    chosen = tuple(range(2, tp_size))
    remote = dict(zip(chosen, partials(chosen)))
    arrivals = []
    for k in range(2, tp_size, 2):
        pair = swap(remote[k + 1], "tp", tp_size, 1)
        summed = (remote[k].astype(F32) + pair.astype(F32)).astype(BF16)
        arrivals.append(swap(summed, "tp", tp_size, k))
    kept, sent = partials((0, 1))
    total = kept.astype(F32) + swap(sent, "tp", tp_size, 1).astype(F32)
    for arrival in arrivals:
        total = total + arrival.astype(F32)
    return total.astype(BF16)


def solution(mesh):
    in_specs = (
        P("sp", "tp"), P(), P(None, "tp"), P(None, "tp"), P(None, "tp"), P(None, "tp"),
        P(None, "tp"), P(None, "tp"), P(None, "tp"), P(None, "tp"), P("tp"), P("sp", "tp"),
        P("tp"), P(), P("tp", None), P("tp", None),
    )
    body = functools.partial(per_device, sp_size=mesh.shape["sp"], tp_size=mesh.shape["tp"])
    return jax.shard_map(
        body, mesh=mesh, in_specs=in_specs, out_specs=P("sp", "tp"), check_vma=False
    )
```
